32 devices in a mesh: sp: 8 (over z, x), tp: 4 (over y, core).
Axes of the slice: x: 2, y: 2, z: 4, core: 2. Of those that a mesh axis runs over, the one named last changes fastest.
Arguments:
- queries: bfloat16 [1024, 32, 128], P('sp', 'tp'), may hold values from -6 to 6
- keys: bfloat16 [1024, 8, 128], P('sp', 'tp'), may hold values from -6 to 6
- values: bfloat16 [1024, 8, 128], P('sp', 'tp'), may hold values from -6 to 6
- q_gain: float32 [128], replicated, may hold values from 0.2 to 8
- k_gain: float32 [128], replicated, may hold values from 0.2 to 8
- w_out: bfloat16 [4096, 2048], P('tp'), may hold values from -0.09375 to 0.09375
- residual: bfloat16 [1024, 2048], P(('sp', 'tp')), may hold values from -6 to 6
- gain_mix: float32 [2048], replicated, may hold values from 0.1 to 1.9
- gain_pre: float32 [2048], replicated, may hold values from 0.1 to 1.9
- routes: int32 [1024, 4], P(('sp', 'tp')), may hold values from 0 to 7, all different within a row; in each aligned block of 32 rows (0 to 31, 32 to 63, ...) at most 32 rows name the same one
- route_weights: float32 [1024, 4], P(('sp', 'tp')), may hold values from 0.1 to 1
- w_gate: bfloat16 [8, 2048, 2048], P('sp', None, 'tp'), may hold values from -0.5 to 0.5
- w_up: bfloat16 [8, 2048, 2048], P('sp', None, 'tp'), may hold values from -0.5 to 0.5
- w_down: bfloat16 [8, 2048, 2048], P('sp', 'tp'), may hold values from -0.125 to 0.125
- gain_moe: float32 [2048], replicated, may hold values from 0.1 to 1.9
Outputs:
- layer_out: bfloat16 [1024, 2048], P(('sp', 'tp'))
The draws below stay inside these ranges and needn't reach their ends.
Inputs may be any that keep to these rules, and one draw needn't show every extreme that they name: `routes`: each row names 4 different experts. In each aligned block of 32 rows (the rows of one device) no expert is named by more than 32 rows, a bound that some block reaches.
All inputs are finite; a program needn't handle non-finite values.
Results may differ from the reference program's by a relative error of at most 0.017.
The reference program's roundings to bfloat16 on the way count: a program that leaves them out, or rounds other values in their place, can miss the bound.
Values may be sent and summed in bfloat16 or wider, within the bound.
No kernel may reach another device: no remote copies, remote signals or barrier semaphores. Data moves between devices by JAX's collectives and lax.ppermute only.
A program may use at most 128 MiB of HBM per device.

```python
import math
import jax
import jax.numpy as jnp
import numpy as np
from jax import lax

D = 2048
Q_HEADS = 32
KV_HEADS = 8
HD = 128
FF = 2048
TOP = 4
GRID_W = 64
TOKENS = 1024
TOK_TP = 32
EXPERTS = 8
CAP = 32
N_TP = 4


def gain_draw(key):
    return 1.0 + 0.18 * jax.random.truncated_normal(key, -4.0, 4.0, (HD,), jnp.float32)


def draw_q_gain(key, part):
    return gain_draw(jax.random.fold_in(key, 31))


def draw_k_gain(key, part):
    return gain_draw(jax.random.fold_in(key, 57))


def steps_of(own_key, shape, shards, least, high):
    def one(position, blocks):
        draws = jax.random.uniform(jax.random.fold_in(jax.random.fold_in(own_key, 6), position), (blocks,), jnp.float32, least / len(shards), high / len(shards))
        return jnp.repeat(jnp.exp(draws), shape[position] // blocks).reshape((-1,) + (1,) * (len(shape) - position - 1))

    loudness = one(*shards[0])
    for cut in shards[1:]:
        loudness = loudness * one(*cut)
    return loudness


def routed_block(stream_key, own, number, rows, number_of, top, bound, lean):
    order = jax.random.permutation(stream_key, number_of)
    packed, common = shares(number_of, rows * top, bound, lean, True), shares(number_of, rows * top, bound, lean, False)
    places = jnp.arange(number_of)

    def named(lengths, rotation):
        used = int((lengths > 0).sum())
        fixed = max(1, used // 4)
        shifted = fixed + (places - fixed + rotation * (used - fixed)) % max(1, number_of - fixed)
        return jnp.zeros((number_of,), jnp.int32).at[order[jnp.where(places < fixed, places, shifted)]].set(jnp.asarray(lengths, jnp.int32))

    lengths = jnp.where(number % 4 == 0, named(packed, number // 4), named(common, number - number // 4 - 1))
    mixed = jax.random.permutation(jax.random.fold_in(own, 3), number_of)
    donor, taker = mixed[0:number_of // 2 * 2:2], mixed[1:number_of // 2 * 2:2]
    room = jnp.minimum(lengths[donor] - 1, bound - lengths[taker]) // 2
    room = jnp.where((donor == order[0]) | (taker == order[0]) | (lengths[taker] == 0), 0, jnp.maximum(room, 0))
    shifted = jax.random.randint(jax.random.fold_in(own, 4), (number_of // 2,), 0, 1 << 20) % (room + 1)
    lengths = lengths.at[donor].add(-shifted).at[taker].add(shifted)
    members = jnp.searchsorted(jnp.cumsum(lengths), jnp.arange(rows * top), side="right").astype(jnp.int32)
    listing = members.reshape(top, rows).T
    listing = listing[jax.random.permutation(jax.random.fold_in(own, 1), rows)]
    rotation = jax.random.randint(jax.random.fold_in(own, 2), (rows, 1), 0, top)
    return jnp.take_along_axis(listing, (jnp.arange(top)[None, :] + rotation) % top, axis=1)


def shares(amount, total, limit, lean, full):
    portions = [(1 << 20) // math.isqrt(standing ** lean) + 1 for standing in range(1, amount + 1)]
    largest = limit if full else min(limit, max(-(-total // amount), total * portions[0] // sum(portions)))
    least = 1 if total - largest >= amount - 1 else 0
    given, spare = [largest] + [least] * (amount - 1), total - largest - least * (amount - 1)
    while spare > 0:
        free = [i for i in range(1, amount) if given[i] < largest] or [i for i in range(1, amount) if given[i] < limit]
        mass, remaining = sum([portions[i] for i in free]), spare
        for i in free:
            addition = min(limit - given[i], max(1, remaining * portions[i] // mass), spare)
            given[i] = given[i] + addition
            spare = spare - addition
    return np.array(given)


def normal_values(stream_key, dims, spread, limit, shards=(), kind=jnp.bfloat16):
    loudness = steps_of(stream_key, dims, shards, -0.22, 0.18) if shards else 1.0
    values = jax.random.normal(stream_key, dims, jnp.float32) * spread * loudness
    return jnp.minimum(jnp.maximum(values, -limit), limit).astype(kind)


def setup_inputs(seed: int = 0) -> dict:
    key_of = jax.random.split(jax.random.key(seed), 16)
    queries = normal_values(key_of[0], (TOKENS, Q_HEADS, HD), 1.0, 6.0, ((0, 8), (1, 4)))
    keys = normal_values(key_of[1], (TOKENS, KV_HEADS, HD), 1.0, 6.0, ((0, 8), (1, 4)))
    values = normal_values(key_of[2], (TOKENS, KV_HEADS, HD), 1.0, 6.0, ((0, 8), (1, 4)))
    q_gain = draw_q_gain(jax.random.fold_in(key_of[15], 71), 0)
    k_gain = draw_k_gain(jax.random.fold_in(key_of[15], 71), 0)
    w_out = normal_values(key_of[5], (Q_HEADS * HD, D), (Q_HEADS * HD) ** -0.5, 0.09375, ((0, 4),))
    residual = normal_values(key_of[6], (TOKENS, D), 1.0, 6.0, ((0, 32),))
    gain_mix = jnp.clip(1.0 + 0.18 * jax.random.normal(key_of[7], (D,), jnp.float32), 0.1, 1.9)
    gain_pre = jnp.clip(1.0 + 0.18 * jax.random.normal(key_of[8], (D,), jnp.float32), 0.1, 1.9)
    routes_keys = jax.random.split(jax.random.fold_in(key_of[9], 1), TOKENS // TOK_TP)
    routes_turns = jax.random.permutation(jax.random.fold_in(key_of[9], 3), TOKENS // TOK_TP)
    routes = jax.vmap(lambda own, number: routed_block(jax.random.fold_in(key_of[9], 2), own, number, TOK_TP, EXPERTS, TOP, CAP, 1))(routes_keys, routes_turns).reshape((TOKENS, TOP))
    route_weights = jnp.clip(jnp.exp(math.log(1.0) - 2.3025851 * jax.random.uniform(key_of[10], (TOKENS, TOP), jnp.float32) ** steps_of(key_of[10], (TOKENS, TOP), ((0, 32),), -0.2, 0.2)), 0.1, 1.0)
    w_gate = normal_values(key_of[11], (EXPERTS, D, FF), (D // 16) ** -0.5, 0.5, ((0, 8), (2, 4)))
    w_up = normal_values(key_of[12], (EXPERTS, D, FF), (D // 16) ** -0.5, 0.5, ((0, 8), (2, 4)))
    w_down = normal_values(key_of[13], (EXPERTS, FF, D), FF ** -0.5, 0.125, ((0, 8), (1, 4)))
    gain_moe = jnp.clip(1.0 + 0.18 * jax.random.normal(key_of[14], (D,), jnp.float32), 0.1, 1.9)
    return {"queries": queries, "keys": keys, "values": values, "q_gain": q_gain, "k_gain": k_gain, "w_out": w_out, "residual": residual, "gain_mix": gain_mix, "gain_pre": gain_pre, "routes": routes, "route_weights": route_weights, "w_gate": w_gate, "w_up": w_up, "w_down": w_down, "gain_moe": gain_moe}


norm_eps = 1e-06
rope_theta = 10000.0
clamp_limit = 7.0
swish_alpha = 1.702

def rope_tables(positions, head_size):
    row_index = (positions // GRID_W).astype(jnp.float32)
    col_index = (positions % GRID_W).astype(jnp.float32)
    freq_count = head_size // 4
    inverse = rope_theta ** (-jnp.arange(freq_count, dtype=jnp.float32) / freq_count)
    angles = jnp.stack([row_index[:, None] * inverse, col_index[:, None] * inverse], axis=1)
    return (jnp.cos(angles), jnp.sin(angles))

def turn(array_in, cosine_table, sine_table):
    token_count, head_count, head_size = array_in.shape
    split_field = array_in.reshape(token_count, head_count, 2, 2, head_size // 4)
    first_half = split_field[:, :, :, 0, :]
    second_half = split_field[:, :, :, 1, :]
    cos_wide = cosine_table[:, None]
    sin_wide = sine_table[:, None]
    turned = jnp.stack([first_half * cos_wide - second_half * sin_wide, second_half * cos_wide + first_half * sin_wide], axis=3)
    return turned.reshape(token_count, head_count, head_size)

def scale_rows(array_in, gain_vec):
    return array_in * lax.rsqrt(lax.optimization_barrier(jnp.mean(array_in * array_in, axis=-1, keepdims=True)) + norm_eps) * gain_vec

def reference(queries, keys, values, q_gain, k_gain, w_out, residual, gain_mix, gain_pre, routes, route_weights, w_gate, w_up, w_down, gain_moe):
    positions = jnp.arange(TOKENS, dtype=jnp.int32)
    cosine_table, sine_table = rope_tables(positions, HD)
    q_turned = (turn(scale_rows(queries.astype(jnp.float32), q_gain), cosine_table, sine_table) * HD ** (-0.5)).astype(jnp.bfloat16)
    k_turned = turn(scale_rows(keys.astype(jnp.float32), k_gain), cosine_table, sine_table).astype(jnp.bfloat16)
    group_size = Q_HEADS // KV_HEADS
    qblock = math.gcd(TOKENS, 512)
    blocks = q_turned.reshape(TOKENS // qblock, qblock, KV_HEADS, group_size, HD)
    k_wide = k_turned.astype(jnp.float32)
    v_wide = values.astype(jnp.float32)

    def attend(block):
        scores = jnp.einsum('qkgd,skd->kgqs', block.astype(jnp.float32), k_wide)
        unnorm = jnp.exp(scores - lax.optimization_barrier(jnp.max(scores, axis=-1, keepdims=True)))
        totals = lax.optimization_barrier(jnp.sum(unnorm, axis=-1))
        summed = jnp.einsum('kgqs,skd->qkgd', unnorm.astype(jnp.bfloat16).astype(jnp.float32), v_wide)
        return (summed / jnp.moveaxis(totals, 2, 0)[..., None]).astype(jnp.bfloat16)
    mixed_heads = lax.map(attend, blocks).reshape(TOKENS, Q_HEADS * HD)
    projected = jnp.dot(mixed_heads, w_out, preferred_element_type=jnp.float32)
    middle = residual.astype(jnp.float32) + scale_rows(projected, gain_mix)
    normed = scale_rows(middle, gain_pre).astype(jnp.bfloat16)
    block_count = TOKENS // TOK_TP
    assign = TOK_TP * TOP
    flat_routes = routes.reshape(block_count, assign)
    expert_hits = (flat_routes[:, :, None] == jnp.arange(EXPERTS, dtype=jnp.int32)[None, None, :]).astype(jnp.int32)
    slot_index = lax.optimization_barrier(jnp.sum((jnp.cumsum(expert_hits, axis=1) - expert_hits) * expert_hits, axis=2)).astype(jnp.int32)
    block_ids = jnp.broadcast_to(jnp.arange(block_count, dtype=jnp.int32)[:, None], (block_count, assign))
    token_ids = (block_ids * TOK_TP + jnp.arange(assign, dtype=jnp.int32)[None, :] // TOP).astype(jnp.int32)
    slot_tokens = jnp.full((EXPERTS, block_count, CAP), TOKENS, jnp.int32).at[flat_routes, block_ids, slot_index].set(token_ids)
    padded = jnp.concatenate([normed, jnp.zeros((1, D), jnp.bfloat16)], axis=0)
    group_width = FF // N_TP

    def serve_expert(expert_args):
        token_rows, gate_weight, up_weight, down_weight = expert_args
        arrived_rows = padded[token_rows.reshape(-1)]
        gate_pre = jnp.minimum(jnp.dot(arrived_rows, gate_weight, preferred_element_type=jnp.float32), clamp_limit)
        up_pre = jnp.clip(jnp.dot(arrived_rows, up_weight, preferred_element_type=jnp.float32), -clamp_limit, clamp_limit)
        active = (gate_pre * jax.nn.sigmoid(swish_alpha * gate_pre) * (up_pre + 1.0)).astype(jnp.bfloat16)
        group_sums = jnp.einsum('rqf,qfd->rqd', active.reshape(-1, N_TP, group_width).astype(jnp.float32), down_weight.reshape(N_TP, group_width, D).astype(jnp.float32))
        group_sums = lax.optimization_barrier(group_sums.astype(jnp.bfloat16)).astype(jnp.float32)
        return lax.optimization_barrier(jnp.sum(group_sums, axis=1)).astype(jnp.bfloat16)
    expert_out = lax.map(serve_expert, (slot_tokens, w_gate, w_up, w_down))
    picked = expert_out.reshape(EXPERTS, block_count, CAP, D)[flat_routes, block_ids, slot_index]
    picked = picked.reshape(TOKENS, TOP, D).astype(jnp.float32)
    mixture = lax.optimization_barrier(jnp.sum(picked * route_weights[:, :, None], axis=1))
    return (middle + scale_rows(mixture, gain_moe)).astype(jnp.bfloat16)
```

```python
import math

import jax
import jax.numpy as jnp
from jax import lax
from jax.sharding import PartitionSpec as P

TOP = 4
GRID_W = 64


norm_eps = 1e-06
rope_theta = 10000.0
clamp_limit = 7.0
swish_alpha = 1.702


def rope_tables(positions, head_size):
    row_index = (positions // GRID_W).astype(jnp.float32)
    col_index = (positions % GRID_W).astype(jnp.float32)
    freq_count = head_size // 4
    inverse = rope_theta ** (-jnp.arange(freq_count, dtype=jnp.float32) / freq_count)
    angles = jnp.stack([row_index[:, None] * inverse, col_index[:, None] * inverse], axis=1)
    return (jnp.cos(angles), jnp.sin(angles))


def turn(array_in, cosine_table, sine_table):
    token_count, head_count, head_size = array_in.shape
    split_field = array_in.reshape(token_count, head_count, 2, 2, head_size // 4)
    first_half = split_field[:, :, :, 0, :]
    second_half = split_field[:, :, :, 1, :]
    cos_wide = cosine_table[:, None]
    sin_wide = sine_table[:, None]
    turned = jnp.stack(
        [
            first_half * cos_wide - second_half * sin_wide,
            second_half * cos_wide + first_half * sin_wide,
        ],
        axis=3,
    )
    return turned.reshape(token_count, head_count, head_size)


def scale_rows(array_in, gain_vec):
    return (
        array_in
        * lax.rsqrt(jnp.mean(array_in * array_in, axis=-1, keepdims=True) + norm_eps)
        * gain_vec
    )


def slot_table(route_rows, experts, capacity):
    flat_routes = route_rows.reshape(-1)
    expert_hits = (flat_routes[:, None] == jnp.arange(experts, dtype=jnp.int32)[None, :]).astype(
        jnp.int32
    )
    slot_index = jnp.sum((jnp.cumsum(expert_hits, axis=0) - expert_hits) * expert_hits, axis=1)
    target = flat_routes * capacity + slot_index
    slot_onehot = target[:, None] == jnp.arange(experts * capacity, dtype=jnp.int32)[None, :]
    return slot_onehot.astype(jnp.bfloat16).reshape(
        route_rows.shape[0], route_rows.shape[1], experts * capacity
    )


def expert_apply(arrived_rows, w_gate, w_up, w_down):
    gate_pre = jnp.minimum(
        jnp.einsum("serd,edf->serf", arrived_rows, w_gate, preferred_element_type=jnp.float32),
        clamp_limit,
    )
    up_pre = jnp.clip(
        jnp.einsum("serd,edf->serf", arrived_rows, w_up, preferred_element_type=jnp.float32),
        -clamp_limit,
        clamp_limit,
    )
    active = (gate_pre * jax.nn.sigmoid(swish_alpha * gate_pre) * (up_pre + 1.0)).astype(
        jnp.bfloat16
    )
    partial_value = jnp.einsum("serf,efd->serd", active, w_down, preferred_element_type=jnp.float32)
    return lax.optimization_barrier(partial_value.astype(jnp.bfloat16)).astype(jnp.float32)


def send_back(finished):
    return lax.all_to_all(finished, "sp", split_axis=0, concat_axis=0, tiled=True)


def chain_shift(array_in, distance, pairs):
    size = lax.axis_size("sp")
    chain = size // pairs
    return lax.ppermute(
        array_in,
        "sp",
        [
            (place * pairs + low, (place + distance) % chain * pairs + low)
            for place in range(chain)
            for low in range(pairs)
        ],
    )


def swap(array_in, axis, bit):
    return lax.ppermute(array_in, axis, [(i, i ^ bit) for i in range(lax.axis_size(axis))])


def swap_x(array_in):
    return swap(array_in, "sp", 1)


def swap_y(array_in):
    return swap(array_in, "tp", 2)


def swap_core(array_in):
    return swap(array_in, "tp", 1)


def chain_gather(array_in):
    chain = lax.axis_size("sp") // 2
    return [array_in] + [chain_shift(array_in, d, 2) for d in range(1, chain)]


def gather_sequence(array_in):
    pieces = chain_gather(array_in)
    first_swap = swap_x(pieces[0])
    others = jnp.concatenate(pieces[1:])
    return jnp.concatenate([pieces[0], others, first_swap, swap_x(others)])


def packed_gates(routes, route_weights, experts_all):
    gates = jnp.sum(
        (routes[:, :, None] == jnp.arange(experts_all, dtype=jnp.int32)).astype(jnp.float32)
        * route_weights[:, :, None],
        axis=1,
    )
    parts = []
    for _ in range(3):
        head = lax.reduce_precision(gates, 8, 7)
        parts.append(head.astype(jnp.bfloat16))
        gates = gates - head
    columns = jnp.concatenate(parts, axis=1)
    lanes = 128
    return jnp.pad(columns, ((0, 0), (0, -columns.shape[1] % lanes)))


def dense_experts(rows, experts_all, w_gate, w_up, w_down):
    local_experts, width = w_gate.shape[0], w_gate.shape[1]
    first = lax.axis_index("sp") * local_experts
    packed = rows[:, width : width + 3 * experts_all].astype(jnp.float32)
    gates = sum(packed[:, i * experts_all : (i + 1) * experts_all] for i in range(3))
    lane = jnp.arange(experts_all, dtype=jnp.int32)[None, :]
    tokens = rows[:, :width]
    total = None
    for e in range(local_experts):
        gate_pre = jnp.minimum(
            jnp.dot(tokens, w_gate[e], preferred_element_type=jnp.float32), clamp_limit
        )
        up_pre = jnp.clip(
            jnp.dot(tokens, w_up[e], preferred_element_type=jnp.float32), -clamp_limit, clamp_limit
        )
        active = (gate_pre * jax.nn.sigmoid(swish_alpha * gate_pre) * (up_pre + 1.0)).astype(
            jnp.bfloat16
        )
        weight = jnp.sum(jnp.where(lane == first + e, gates, 0.0), axis=1, keepdims=True)
        term = jnp.dot(active, w_down[e], preferred_element_type=jnp.float32) * weight
        total = term if total is None else total + term
    return total.astype(jnp.bfloat16)


def added(array_in, arrived):
    return (array_in.astype(jnp.float32) + arrived.astype(jnp.float32)).astype(jnp.bfloat16)


def with_core_rows(parts):
    joined = jnp.concatenate(parts)
    return jnp.concatenate([joined, swap_core(joined)])


def core_sums(chunk):
    kept = chunk.shape[0] // 2
    return added(chunk[:kept], swap_core(chunk[kept:]))


def route_experts(normed, gate_columns, experts_all, w_gate, w_up, w_down):
    def serve(rows):
        return dense_experts(rows, experts_all, w_gate, w_up, w_down)

    half = normed.shape[0] // 2
    pieces = chain_gather(jnp.concatenate([normed, gate_columns], axis=1))
    own_a = jnp.concatenate([piece[:half] for piece in pieces])
    own_b = jnp.concatenate([piece[half:] for piece in pieces])
    x_a, y_b = swap_x(own_a), swap_y(own_b)
    x_b, y_a = swap_x(own_b), swap_y(own_a)
    own_sums = serve(with_core_rows([own_a, own_b]))
    x_a, y_b, own_sums = lax.optimization_barrier((x_a, y_b, own_sums))
    xy_a, xy_b = swap_y(x_a), swap_x(y_b)
    side_sums = serve(with_core_rows([x_a, x_b, y_a, y_b]))
    xy_a, xy_b, side_sums = lax.optimization_barrier((xy_a, xy_b, side_sums))
    far_sums = serve(with_core_rows([xy_a, xy_b]))
    own_a, own_b = jnp.split(core_sums(own_sums), 2)
    x_a, x_b, y_a, y_b = jnp.split(core_sums(side_sums), 4)
    xy_a, xy_b = jnp.split(core_sums(far_sums), 2)
    own_a = added(own_a, swap_y(y_a))
    own_b = added(own_b, swap_x(x_b))
    x_a = added(x_a, swap_y(xy_a))
    y_b = added(y_b, swap_x(xy_b))
    own_a = added(own_a, swap_x(x_a))
    own_b = added(own_b, swap_y(y_b))
    chain = len(pieces)
    back = jnp.concatenate(
        [own_a.reshape(chain, half, -1), own_b.reshape(chain, half, -1)], axis=1
    )
    mixture = back[0].astype(jnp.float32)
    for d in range(1, chain):
        mixture = mixture + chain_shift(back[d], -d, 2).astype(jnp.float32)
    return mixture


def relative_blocks(array_in):
    place = lax.axis_index("tp")
    blocks = array_in.reshape((4, array_in.shape[0] // 4) + array_in.shape[1:])
    return jnp.concatenate(
        [lax.dynamic_index_in_dim(blocks, place ^ r, axis=0, keepdims=False) for r in (1, 3, 0, 2)]
    )


def project_scatter(mixed_heads, w_out):
    partial_rows = jnp.dot(mixed_heads, w_out, preferred_element_type=jnp.float32)
    sent, kept = jnp.split(partial_rows, 2)
    here, away = jnp.split(kept + swap_core(sent.astype(jnp.bfloat16)).astype(jnp.float32), 2)
    return here + swap_y(away.astype(jnp.bfloat16)).astype(jnp.float32)


def on_device(
    queries,
    keys,
    values,
    q_gain,
    k_gain,
    w_out,
    residual,
    gain_mix,
    gain_pre,
    routes,
    route_weights,
    w_gate,
    w_up,
    w_down,
    gain_moe,
):
    tok_rows, head_local, head_size = queries.shape
    kv_local = keys.shape[1]
    group_size = head_local // kv_local
    tok_part = residual.shape[0]
    local_experts = w_gate.shape[0]
    experts_all = local_experts * lax.axis_size("sp")
    capacity = max(2, (2 * tok_part * TOP + experts_all - 1) // experts_all)
    dense = (
        local_experts * capacity >= tok_part
        and lax.axis_size("sp") % 2 == 0
        and lax.axis_size("tp") == 2 * 2
        and tok_part % 2 == 0
        and tok_rows == 4 * tok_part
    )
    positions = lax.axis_index("sp") * tok_rows + jnp.arange(tok_rows, dtype=jnp.int32)
    cosine_table, sine_table = rope_tables(positions, head_size)
    q_turned = (
        turn(scale_rows(queries.astype(jnp.float32), q_gain), cosine_table, sine_table)
        * head_size ** (-0.5)
    ).astype(jnp.bfloat16)
    k_turned = turn(scale_rows(keys.astype(jnp.float32), k_gain), cosine_table, sine_table).astype(
        jnp.bfloat16
    )
    if dense:
        q_turned = relative_blocks(q_turned)
    q_grouped = q_turned.reshape(tok_rows, kv_local, group_size, head_size)
    initial = (
        jnp.full((kv_local, group_size, tok_rows), -jnp.inf, jnp.float32),
        jnp.zeros((kv_local, group_size, tok_rows), jnp.float32),
        jnp.zeros((kv_local, group_size, tok_rows, head_size), jnp.float32),
    )
    carry_state = initial
    if dense:
        gate_columns = packed_gates(routes, route_weights, experts_all)
        key_value = gather_sequence(
            jnp.concatenate(
                [k_turned.reshape(tok_rows, -1), values.reshape(tok_rows, -1)], axis=1
            )
        )
        key_piece, value_piece = jnp.split(key_value, 2, axis=1)
    else:
        key_piece = lax.all_gather(k_turned, "sp", axis=0, tiled=True)
        value_piece = lax.all_gather(values, "sp", axis=0, tiled=True)
    piece_rows = key_piece.shape[0]
    block_rows = math.gcd(piece_rows, 1024)
    key_blocks = key_piece.reshape(piece_rows // block_rows, block_rows, kv_local, head_size)
    value_blocks = value_piece.reshape(piece_rows // block_rows, block_rows, kv_local, head_size)

    def absorb_block(state_now, key_value):
        running_max, running_sum, weighted = state_now
        key_block, value_block = key_value
        scores = jnp.einsum(
            "qkgd,skd->kgqs", q_grouped, key_block, preferred_element_type=jnp.float32
        )
        new_max = jnp.maximum(running_max, jnp.max(scores, axis=-1))
        rescale = jnp.exp(running_max - new_max)
        unnorm = jnp.exp(scores - new_max[..., None])
        running_sum = running_sum * rescale + jnp.sum(unnorm, axis=-1)
        weighted = weighted * rescale[..., None] + jnp.einsum(
            "kgqs,skd->kgqd",
            unnorm.astype(jnp.bfloat16),
            value_block,
            preferred_element_type=jnp.float32,
        )
        return ((new_max, running_sum, weighted), None)

    carry_state, ignored = lax.scan(absorb_block, carry_state, (key_blocks, value_blocks))
    running_max, running_sum, weighted = carry_state
    mixed_heads = (weighted / running_sum[..., None]).transpose(2, 0, 1, 3)
    mixed_heads = mixed_heads.reshape(tok_rows, head_local * head_size).astype(jnp.bfloat16)
    width = residual.shape[1]
    if dense:
        projected = project_scatter(mixed_heads, w_out)
    else:
        projected = lax.psum_scatter(
            jnp.dot(mixed_heads, w_out, preferred_element_type=jnp.float32).astype(jnp.bfloat16),
            "tp",
            scatter_dimension=0,
            tiled=True,
        ).astype(jnp.float32)
    middle = residual.astype(jnp.float32) + scale_rows(projected, gain_mix)
    normed = scale_rows(middle, gain_pre).astype(jnp.bfloat16)
    if dense:
        mixture = route_experts(normed, gate_columns, experts_all, w_gate, w_up, w_down)
        return (middle + scale_rows(mixture, gain_moe)).astype(jnp.bfloat16)
    tables = slot_table(routes, experts_all, capacity)
    chosen = jnp.sum(tables, axis=1)
    outbound = jnp.einsum("tp,td->pd", chosen, normed, preferred_element_type=jnp.float32)
    outbound = outbound.astype(jnp.bfloat16).reshape(experts_all, capacity, width)
    arrived_rows = lax.all_gather(
        lax.all_to_all(outbound, "sp", split_axis=0, concat_axis=0, tiled=True),
        "tp",
        axis=0,
        tiled=True,
    )
    leading = arrived_rows.shape[0] // local_experts
    partial_value = expert_apply(
        arrived_rows.reshape(leading, local_experts, arrived_rows.shape[1], width),
        w_gate,
        w_up,
        w_down,
    )
    summed = lax.psum_scatter(
        partial_value.reshape(arrived_rows.shape).astype(jnp.bfloat16),
        "tp",
        scatter_dimension=0,
        tiled=True,
    )
    returned = send_back(summed)
    gathered = jnp.einsum(
        "tkp,pd->tkd",
        tables,
        returned.reshape(experts_all * capacity, width),
        preferred_element_type=jnp.float32,
    )
    mixture = jnp.sum(gathered * route_weights[:, :, None], axis=1)
    return (middle + scale_rows(mixture, gain_moe)).astype(jnp.bfloat16)


def solution(mesh):
    placed = (
        P("sp", "tp", None),
        P("sp", "tp", None),
        P("sp", "tp", None),
        P(),
        P(),
        P("tp", None),
        P(("sp", "tp"), None),
        P(),
        P(),
        P(("sp", "tp"), None),
        P(("sp", "tp"), None),
        P("sp", None, "tp"),
        P("sp", None, "tp"),
        P("sp", "tp", None),
        P(),
    )
    return jax.shard_map(
        on_device, mesh=mesh, in_specs=placed, out_specs=P(("sp", "tp"), None), check_vma=False
    )
```

```python
import math

import jax
import jax.numpy as jnp
from jax import lax
from jax.sharding import PartitionSpec as P

TOP = 4
GRID_W = 64


norm_eps = 1e-06
rope_theta = 10000.0
clamp_limit = 7.0
swish_alpha = 1.702


def rope_tables(positions, head_size):
    row_index = (positions // GRID_W).astype(jnp.float32)
    col_index = (positions % GRID_W).astype(jnp.float32)
    freq_count = head_size // 4
    inverse = rope_theta ** (-jnp.arange(freq_count, dtype=jnp.float32) / freq_count)
    angles = jnp.stack([row_index[:, None] * inverse, col_index[:, None] * inverse], axis=1)
    return (jnp.cos(angles), jnp.sin(angles))


def turn(array_in, cosine_table, sine_table):
    token_count, head_count, head_size = array_in.shape
    split_field = array_in.reshape(token_count, head_count, 2, 2, head_size // 4)
    first_half = split_field[:, :, :, 0, :]
    second_half = split_field[:, :, :, 1, :]
    cos_wide = cosine_table[:, None]
    sin_wide = sine_table[:, None]
    turned = jnp.stack(
        [
            first_half * cos_wide - second_half * sin_wide,
            second_half * cos_wide + first_half * sin_wide,
        ],
        axis=3,
    )
    return turned.reshape(token_count, head_count, head_size)


def scale_rows(array_in, gain_vec):
    return (
        array_in
        * lax.rsqrt(jnp.mean(array_in * array_in, axis=-1, keepdims=True) + norm_eps)
        * gain_vec
    )


def slot_table(route_rows, experts, capacity):
    flat_routes = route_rows.reshape(-1)
    expert_hits = (flat_routes[:, None] == jnp.arange(experts, dtype=jnp.int32)[None, :]).astype(
        jnp.int32
    )
    slot_index = jnp.sum((jnp.cumsum(expert_hits, axis=0) - expert_hits) * expert_hits, axis=1)
    target = flat_routes * capacity + slot_index
    slot_onehot = target[:, None] == jnp.arange(experts * capacity, dtype=jnp.int32)[None, :]
    return slot_onehot.astype(jnp.bfloat16).reshape(
        route_rows.shape[0], route_rows.shape[1], experts * capacity
    )


def expert_apply(arrived_rows, w_gate, w_up, w_down):
    gate_pre = jnp.minimum(
        jnp.einsum("serd,edf->serf", arrived_rows, w_gate, preferred_element_type=jnp.float32),
        clamp_limit,
    )
    up_pre = jnp.clip(
        jnp.einsum("serd,edf->serf", arrived_rows, w_up, preferred_element_type=jnp.float32),
        -clamp_limit,
        clamp_limit,
    )
    active = (gate_pre * jax.nn.sigmoid(swish_alpha * gate_pre) * (up_pre + 1.0)).astype(
        jnp.bfloat16
    )
    partial_value = jnp.einsum("serf,efd->serd", active, w_down, preferred_element_type=jnp.float32)
    return lax.optimization_barrier(partial_value.astype(jnp.bfloat16)).astype(jnp.float32)


def send_back(finished):
    return lax.all_to_all(finished, "sp", split_axis=0, concat_axis=0, tiled=True)


def swap(array_in, axis, bit):
    return lax.ppermute(array_in, axis, [(i, i ^ bit) for i in range(lax.axis_size(axis))])


def swap_x(array_in):
    return swap(array_in, "sp", 1)


def swap_y(array_in):
    return swap(array_in, "tp", 2)


def swap_core(array_in):
    return swap(array_in, "tp", 1)


def swap_chain(array_in, distance):
    return swap(array_in, "sp", 2 * distance)


def chain_gather(array_in):
    chain = lax.axis_size("sp") // 2
    return [array_in] + [swap_chain(array_in, d) for d in range(1, chain)]


def gather_sequence(array_in):
    pieces = chain_gather(array_in)
    return jnp.concatenate(pieces + [swap_x(piece) for piece in pieces])


def packed_gates(routes, route_weights, experts_all):
    gates = jnp.sum(
        (routes[:, :, None] == jnp.arange(experts_all, dtype=jnp.int32)).astype(jnp.float32)
        * route_weights[:, :, None],
        axis=1,
    )
    parts = []
    for _ in range(3):
        head = lax.reduce_precision(gates, 8, 7)
        parts.append(head.astype(jnp.bfloat16))
        gates = gates - head
    columns = jnp.concatenate(parts, axis=1)
    lanes = 128
    return jnp.pad(columns, ((0, 0), (0, -columns.shape[1] % lanes)))


def dense_experts(rows, experts_all, w_both, w_down):
    local_experts, width = w_both.shape[0], w_both.shape[1]
    first = lax.axis_index("sp") * local_experts
    packed = rows[:, width : width + 3 * experts_all].astype(jnp.float32)
    gates = sum(packed[:, i * experts_all : (i + 1) * experts_all] for i in range(3))
    lane = jnp.arange(experts_all, dtype=jnp.int32)[None, :]
    tokens = rows[:, :width]
    total = None
    for e in range(local_experts):
        both = jnp.dot(tokens, w_both[e], preferred_element_type=jnp.float32)
        gate_pre, up_pre = jnp.split(both, 2, axis=1)
        gate_pre = jnp.minimum(gate_pre, clamp_limit)
        up_pre = jnp.clip(up_pre, -clamp_limit, clamp_limit)
        active = (gate_pre * jax.nn.sigmoid(swish_alpha * gate_pre) * (up_pre + 1.0)).astype(
            jnp.bfloat16
        )
        weight = jnp.sum(jnp.where(lane == first + e, gates, 0.0), axis=1, keepdims=True)
        term = jnp.dot(active, w_down[e], preferred_element_type=jnp.float32) * weight
        total = term if total is None else total + term
    return total.astype(jnp.bfloat16)


def added(array_in, arrived):
    return (array_in.astype(jnp.float32) + arrived.astype(jnp.float32)).astype(jnp.bfloat16)


def with_core_rows(parts):
    joined = jnp.concatenate(parts)
    return jnp.concatenate([joined, swap_core(joined)])


def core_sums(chunk):
    kept = chunk.shape[0] // 2
    return added(chunk[:kept], swap_core(chunk[kept:]))


def route_experts(normed, gate_columns, experts_all, w_both, w_down):
    def serve(rows):
        return dense_experts(rows, experts_all, w_both, w_down)

    half = normed.shape[0] // 2
    extended = jnp.concatenate([normed, gate_columns], axis=1)
    pieces = chain_gather(extended[:half])
    own_a = jnp.concatenate(pieces)
    x_a, y_a = swap_x(own_a), swap_y(own_a)
    own_b = jnp.concatenate(chain_gather(extended[half:]))
    x_b, y_b = swap_x(own_b), swap_y(own_b)
    own_sums = serve(with_core_rows([own_a, own_b]))
    xy_a, xy_b = swap_y(x_a), swap_x(y_b)
    side_sums = serve(
        with_core_rows(lax.optimization_barrier((x_a, y_a, x_b, y_b, own_sums))[:4])
    )
    far_sums = serve(with_core_rows(lax.optimization_barrier((xy_a, xy_b, side_sums))[:2]))
    x_a, y_a, x_b, y_b = jnp.split(core_sums(side_sums), 4)
    own_a, own_b = jnp.split(core_sums(own_sums), 2)
    xy_a, xy_b = jnp.split(core_sums(far_sums), 2)
    own_a = added(own_a, swap_y(y_a))
    own_b = added(own_b, swap_x(x_b))
    x_a = added(x_a, swap_y(xy_a))
    y_b = added(y_b, swap_x(xy_b))
    own_a = added(own_a, swap_x(x_a))
    own_b = added(own_b, swap_y(y_b))
    chain = len(pieces)
    back = jnp.concatenate(
        [own_a.reshape(chain, half, -1), own_b.reshape(chain, half, -1)], axis=1
    )
    mixture = back[0].astype(jnp.float32)
    for d in range(1, chain):
        mixture = mixture + swap_chain(back[d], d).astype(jnp.float32)
    return mixture


def relative_blocks(array_in):
    place = lax.axis_index("tp")
    size = array_in.shape[0] // 4
    return jnp.concatenate(
        [lax.dynamic_slice_in_dim(array_in, (place ^ r) * size, size) for r in (1, 3, 0, 2)]
    )


def project_scatter(mixed_heads, w_out):
    partial_rows = jnp.dot(mixed_heads, w_out, preferred_element_type=jnp.float32)
    sent, kept = jnp.split(partial_rows, 2)
    here, away = jnp.split(kept + swap_core(sent.astype(jnp.bfloat16)).astype(jnp.float32), 2)
    return here + swap_y(away.astype(jnp.bfloat16)).astype(jnp.float32)


def on_device(
    queries,
    keys,
    values,
    q_gain,
    k_gain,
    w_out,
    residual,
    gain_mix,
    gain_pre,
    routes,
    route_weights,
    w_gate,
    w_up,
    w_down,
    gain_moe,
):
    tok_rows, head_local, head_size = queries.shape
    kv_local = keys.shape[1]
    group_size = head_local // kv_local
    tok_part = residual.shape[0]
    local_experts = w_gate.shape[0]
    experts_all = local_experts * lax.axis_size("sp")
    capacity = max(2, (2 * tok_part * TOP + experts_all - 1) // experts_all)
    dense = (
        local_experts * capacity >= tok_part
        and lax.axis_size("sp") & (lax.axis_size("sp") - 1) == 0
        and lax.axis_size("sp") > 2
        and lax.axis_size("tp") == 2 * 2
        and tok_part % 2 == 0
        and tok_rows == 4 * tok_part
    )
    positions = lax.axis_index("sp") * tok_rows + jnp.arange(tok_rows, dtype=jnp.int32)
    cosine_table, sine_table = rope_tables(positions, head_size)
    query_cosine, query_sine = cosine_table, sine_table
    if dense:
        w_both = lax.optimization_barrier(jnp.concatenate([w_gate, w_up], axis=2))
        queries = relative_blocks(queries)
        query_cosine, query_sine = rope_tables(relative_blocks(positions), head_size)
    q_turned = (
        turn(scale_rows(queries.astype(jnp.float32), q_gain), query_cosine, query_sine)
        * head_size ** (-0.5)
    ).astype(jnp.bfloat16)
    k_turned = turn(scale_rows(keys.astype(jnp.float32), k_gain), cosine_table, sine_table).astype(
        jnp.bfloat16
    )
    q_grouped = q_turned.reshape(tok_rows, kv_local, group_size, head_size)
    initial = (
        jnp.full((kv_local, group_size, tok_rows), -jnp.inf, jnp.float32),
        jnp.zeros((kv_local, group_size, tok_rows), jnp.float32),
        jnp.zeros((kv_local, group_size, tok_rows, head_size), jnp.float32),
    )
    carry_state = initial
    if dense:
        gate_columns = packed_gates(routes, route_weights, experts_all)
        key_value = gather_sequence(
            jnp.concatenate(
                [k_turned.reshape(tok_rows, -1), values.reshape(tok_rows, -1)], axis=1
            )
        )
        key_piece, value_piece = jnp.split(key_value, 2, axis=1)
    else:
        key_piece = lax.all_gather(k_turned, "sp", axis=0, tiled=True)
        value_piece = lax.all_gather(values, "sp", axis=0, tiled=True)
    piece_rows = key_piece.shape[0]
    block_rows = math.gcd(piece_rows, 1024)
    key_blocks = key_piece.reshape(piece_rows // block_rows, block_rows, kv_local, head_size)
    value_blocks = value_piece.reshape(piece_rows // block_rows, block_rows, kv_local, head_size)

    def absorb_block(state_now, key_value):
        running_max, running_sum, weighted = state_now
        key_block, value_block = key_value
        scores = jnp.einsum(
            "qkgd,skd->kgqs", q_grouped, key_block, preferred_element_type=jnp.float32
        )
        new_max = jnp.maximum(running_max, jnp.max(scores, axis=-1))
        rescale = jnp.exp(running_max - new_max)
        unnorm = jnp.exp(scores - new_max[..., None])
        running_sum = running_sum * rescale + jnp.sum(unnorm, axis=-1)
        weighted = weighted * rescale[..., None] + jnp.einsum(
            "kgqs,skd->kgqd",
            unnorm.astype(jnp.bfloat16),
            value_block,
            preferred_element_type=jnp.float32,
        )
        return ((new_max, running_sum, weighted), None)

    carry_state, ignored = lax.scan(absorb_block, carry_state, (key_blocks, value_blocks))
    running_max, running_sum, weighted = carry_state
    mixed_heads = (weighted / running_sum[..., None]).transpose(2, 0, 1, 3)
    mixed_heads = mixed_heads.reshape(tok_rows, head_local * head_size).astype(jnp.bfloat16)
    width = residual.shape[1]
    if dense:
        projected = project_scatter(mixed_heads, w_out)
    else:
        projected = lax.psum_scatter(
            jnp.dot(mixed_heads, w_out, preferred_element_type=jnp.float32).astype(jnp.bfloat16),
            "tp",
            scatter_dimension=0,
            tiled=True,
        ).astype(jnp.float32)
    middle = residual.astype(jnp.float32) + scale_rows(projected, gain_mix)
    normed = scale_rows(middle, gain_pre).astype(jnp.bfloat16)
    if dense:
        mixture = route_experts(normed, gate_columns, experts_all, w_both, w_down)
        return (middle + scale_rows(mixture, gain_moe)).astype(jnp.bfloat16)
    tables = slot_table(routes, experts_all, capacity)
    chosen = jnp.sum(tables, axis=1)
    outbound = jnp.einsum("tp,td->pd", chosen, normed, preferred_element_type=jnp.float32)
    outbound = outbound.astype(jnp.bfloat16).reshape(experts_all, capacity, width)
    arrived_rows = lax.all_gather(
        lax.all_to_all(outbound, "sp", split_axis=0, concat_axis=0, tiled=True),
        "tp",
        axis=0,
        tiled=True,
    )
    leading = arrived_rows.shape[0] // local_experts
    partial_value = expert_apply(
        arrived_rows.reshape(leading, local_experts, arrived_rows.shape[1], width),
        w_gate,
        w_up,
        w_down,
    )
    summed = lax.psum_scatter(
        partial_value.reshape(arrived_rows.shape).astype(jnp.bfloat16),
        "tp",
        scatter_dimension=0,
        tiled=True,
    )
    returned = send_back(summed)
    gathered = jnp.einsum(
        "tkp,pd->tkd",
        tables,
        returned.reshape(experts_all * capacity, width),
        preferred_element_type=jnp.float32,
    )
    mixture = jnp.sum(gathered * route_weights[:, :, None], axis=1)
    return (middle + scale_rows(mixture, gain_moe)).astype(jnp.bfloat16)


def solution(mesh):
    placed = (
        P("sp", "tp", None),
        P("sp", "tp", None),
        P("sp", "tp", None),
        P(),
        P(),
        P("tp", None),
        P(("sp", "tp"), None),
        P(),
        P(),
        P(("sp", "tp"), None),
        P(("sp", "tp"), None),
        P("sp", None, "tp"),
        P("sp", None, "tp"),
        P("sp", "tp", None),
        P(),
    )
    return jax.shard_map(
        on_device, mesh=mesh, in_specs=placed, out_specs=P(("sp", "tp"), None), check_vma=False
    )
```
